32 devices in a mesh: fs: 8 (over z, x), tp: 4 (over y, core).
Axes of the slice: x: 2, y: 2, z: 4, core: 2. Of those that a mesh axis runs over, the one named last changes fastest.
Arguments:
- mixer_input: bfloat16 [8192, 4096], P('fs'), may hold values from -6 to 6
- cell_output: bfloat16 [8192, 2048], P('fs'), may hold values from -6 to 6
- query_grad: bfloat16 [8192, 2048], P('fs', 'tp'), may hold values from -4 to 4
- value_grad: bfloat16 [8192, 2048], P('fs', 'tp'), may hold values from -4 to 4
- output_grad: bfloat16 [8192, 4096], P('fs', 'tp'), may hold values from -4 to 4
- query_weight: float32 [4096, 2048], P('fs', 'tp'), may hold values from -6 to 6
- value_weight: float32 [4096, 2048], P('fs', 'tp'), may hold values from -6 to 6
- output_weight: float32 [2048, 4096], P('fs', 'tp'), may hold values from -6 to 6
- query_basis: bfloat16 [4096, 128], P('fs'), may hold values from -0.09375 to 0.09375
- value_basis: bfloat16 [4096, 128], P('fs'), may hold values from -0.09375 to 0.09375
- output_basis: bfloat16 [2048, 128], P('fs'), may hold values from -0.125 to 0.125
- query_mean: float32 [128, 2048], P(None, 'tp'), may hold values from -6 to 6
- value_mean: float32 [128, 2048], P(None, 'tp'), may hold values from -6 to 6
- output_mean: float32 [128, 4096], P(None, 'tp'), may hold values from -6 to 6
- query_square: float32 [128, 2048], P(None, 'tp'), may hold values from 0.25 to 4
- value_square: float32 [128, 2048], P(None, 'tp'), may hold values from 0.25 to 4
- output_square: float32 [128, 4096], P(None, 'tp'), may hold values from 0.25 to 4
Outputs:
- query_step: float32 [4096, 2048], P('fs', 'tp')
- value_step: float32 [4096, 2048], P('fs', 'tp')
- output_step: float32 [2048, 4096], P('fs', 'tp')
- query_copy: bfloat16 [4096, 2048], P(None, 'tp')
- value_copy: bfloat16 [4096, 2048], P(None, 'tp')
- output_copy: bfloat16 [2048, 4096], P(None, 'tp')
- query_first: float32 [128, 2048], P(None, 'tp')
- value_first: float32 [128, 2048], P(None, 'tp')
- output_first: float32 [128, 4096], P(None, 'tp')
- query_second: float32 [128, 2048], P(None, 'tp')
- value_second: float32 [128, 2048], P(None, 'tp')
- output_second: float32 [128, 4096], P(None, 'tp')
The draws below stay inside these ranges and needn't reach their ends.
All inputs are finite; a program needn't handle non-finite values.
Results may differ from the reference program's by a relative error of at most 0.013.
Values may be sent and summed in bfloat16 or wider, within the bound.
No kernel may reach another device: no remote copies, remote signals or barrier semaphores. Data moves between devices by JAX's collectives and lax.ppermute only.
A program may use at most 128 MiB of HBM per device.

```python
import math
import jax
import jax.numpy as jnp
from jax import lax

MODEL = 4096
CELL = 2048
RANK = 128
TOKENS = 8192


def input_rows(key):
    return jnp.clip(jax.random.normal(jax.random.fold_in(key, 101), (TOKENS, MODEL), jnp.float32), -6.0, 6.0)


def readout_rows(key):
    return jnp.clip(jax.random.normal(jax.random.fold_in(key, 102), (TOKENS, CELL), jnp.float32), -6.0, 6.0)


def coherent_grad(key, rows, salt, width):
    inner = rows.shape[1]
    noise = jnp.clip(jax.random.normal(jax.random.fold_in(key, salt), (TOKENS, width), jnp.float32), -6.0, 6.0) * (1.0 / math.sqrt(TOKENS))
    heading = jax.random.normal(jax.random.fold_in(key, salt + 1), (inner,), jnp.float32) * (1.0 / math.sqrt(inner))
    column = jnp.clip(jax.random.normal(jax.random.fold_in(key, salt + 2), (width,), jnp.float32), -3.0, 3.0)
    strength = 4.0 * math.sqrt(inner) / TOKENS
    along = jnp.dot(rows, heading, precision=lax.Precision.HIGHEST)
    return jnp.clip(noise + strength * along[:, None] * column[None, :], -4.0, 4.0)


def draw_mixer_input(key, part):
    return input_rows(key).astype(jnp.bfloat16)


def draw_cell_output(key, part):
    return readout_rows(key).astype(jnp.bfloat16)


def draw_query_grad(key, part):
    return coherent_grad(key, input_rows(key), 201, CELL).astype(jnp.bfloat16)


def draw_value_grad(key, part):
    return coherent_grad(key, input_rows(key), 211, CELL).astype(jnp.bfloat16)


def draw_output_grad(key, part):
    return coherent_grad(key, readout_rows(key), 221, MODEL).astype(jnp.bfloat16)


def shard_levels(key, dims, pieces, low, high):
    level, own = 1.0, jax.random.fold_in(key, 6)
    for axis_at, blocks in pieces:
        heights = jnp.exp(jax.random.uniform(jax.random.fold_in(own, axis_at), (blocks,), jnp.float32, low / len(pieces), high / len(pieces)))
        level = level * jnp.repeat(heights, dims[axis_at] // blocks).reshape([-1 if axis == axis_at else 1 for axis in range(len(dims))])
    return level


def gaussian(own_key, extent, deviation, reach, cuts=(), kind=jnp.bfloat16):
    array = deviation * jax.random.normal(own_key, extent, jnp.float32)
    if cuts:
        array = array * shard_levels(own_key, extent, cuts, -0.22, 0.18)
    return jnp.clip(array, -reach, reach).astype(kind)


def setup_inputs(seed: int = 0) -> dict:
    seeds = jax.random.split(jax.random.key(seed), 18)
    return {
        "mixer_input": draw_mixer_input(jax.random.fold_in(seeds[17], 71), 0),
        "cell_output": draw_cell_output(jax.random.fold_in(seeds[17], 71), 0),
        "query_grad": draw_query_grad(jax.random.fold_in(seeds[17], 71), 0),
        "value_grad": draw_value_grad(jax.random.fold_in(seeds[17], 71), 0),
        "output_grad": draw_output_grad(jax.random.fold_in(seeds[17], 71), 0),
        "query_weight": gaussian(seeds[5], (MODEL, CELL), 1.0, 6.0, ((0, 8), (1, 4)), jnp.float32),
        "value_weight": gaussian(seeds[6], (MODEL, CELL), 1.0, 6.0, ((0, 8), (1, 4)), jnp.float32),
        "output_weight": gaussian(seeds[7], (CELL, MODEL), 1.0, 6.0, ((0, 8), (1, 4)), jnp.float32),
        "query_basis": gaussian(seeds[8], (MODEL, RANK), MODEL ** -0.5, 0.09375, ((0, 8),)),
        "value_basis": gaussian(seeds[9], (MODEL, RANK), MODEL ** -0.5, 0.09375, ((0, 8),)),
        "output_basis": gaussian(seeds[10], (CELL, RANK), CELL ** -0.5, 0.125, ((0, 8),)),
        "query_mean": gaussian(seeds[11], (RANK, CELL), 1.0, 6.0, ((1, 4),), jnp.float32),
        "value_mean": gaussian(seeds[12], (RANK, CELL), 1.0, 6.0, ((1, 4),), jnp.float32),
        "output_mean": gaussian(seeds[13], (RANK, MODEL), 1.0, 6.0, ((1, 4),), jnp.float32),
        "query_square": jnp.clip(jnp.exp(math.log(4.0) - 2.7725887 * jax.random.uniform(seeds[14], (RANK, CELL), jnp.float32) ** shard_levels(seeds[14], (RANK, CELL), ((1, 4),), -0.2, 0.2)), 0.25, 4.0),
        "value_square": jnp.clip(jnp.exp(math.log(4.0) - 2.7725887 * jax.random.uniform(seeds[15], (RANK, CELL), jnp.float32) ** shard_levels(seeds[15], (RANK, CELL), ((1, 4),), -0.2, 0.2)), 0.25, 4.0),
        "output_square": jnp.clip(jnp.exp(math.log(4.0) - 2.7725887 * jax.random.uniform(seeds[16], (RANK, MODEL), jnp.float32) ** shard_levels(seeds[16], (RANK, MODEL), ((1, 4),), -0.2, 0.2)), 0.25, 4.0),
    }


beta_first = 0.8
beta_second = 0.9
floor_mean = 0.005
learn_rate = 0.05

def across(leading, trailing):
    return lax.dot_general(leading, trailing, (((0,), (0,)), ((), ())), preferred_element_type=jnp.float32)

def moments(gradient, basis, mean_old, square_old):
    factor_full = basis.astype(jnp.float32)
    projected = lax.dot_general(factor_full, gradient, (((0,), (0,)), ((), ())), precision=lax.Precision.HIGHEST, preferred_element_type=jnp.float32)
    moment_one = beta_first * mean_old + (1.0 - beta_first) * projected
    moment_two = beta_second * square_old + (1.0 - beta_second) * projected * projected
    direction = moment_one / jnp.sqrt(moment_two)
    lowrank = jnp.dot(factor_full, direction, precision=lax.Precision.HIGHEST, preferred_element_type=jnp.float32)
    return (lowrank, moment_one, moment_two)

def reference(mixer_input, cell_output, query_grad, value_grad, output_grad, query_weight, value_weight, output_weight, query_basis, value_basis, output_basis, query_mean, value_mean, output_mean, query_square, value_square, output_square):
    gradient_query = across(mixer_input, query_grad)
    gradient_value = across(mixer_input, value_grad)
    gradient_output = across(cell_output, output_grad)
    low_query, query_first, query_second = moments(gradient_query, query_basis, query_mean, query_square)
    low_value, value_first, value_second = moments(gradient_value, value_basis, value_mean, value_square)
    low_output, output_first, output_second = moments(gradient_output, output_basis, output_mean, output_square)
    squares = jnp.sum(low_query * low_query) + jnp.sum(low_value * low_value) + jnp.sum(low_output * low_output)
    factor = 1.0 / jnp.sqrt(squares / (3.0 * MODEL * CELL) + floor_mean)
    query_step = -factor * low_query
    value_step = -factor * low_value
    output_step = -factor * low_output
    query_copy = (query_weight + learn_rate * query_step).astype(jnp.bfloat16)
    value_copy = (value_weight + learn_rate * value_step).astype(jnp.bfloat16)
    output_copy = (output_weight + learn_rate * output_step).astype(jnp.bfloat16)
    return (query_step, value_step, output_step, query_copy, value_copy, output_copy, query_first, value_first, output_first, query_second, value_second, output_second)
```

```python
import jax
import jax.numpy as jnp
from jax import lax
from jax.experimental import pallas as pl
from jax.experimental.pallas import tpu as pltpu
from jax.sharding import PartitionSpec as P

beta_first = 0.8
beta_second = 0.9
floor_mean = 0.005
learn_rate = 0.05

STREAMS = 2
BF = jnp.bfloat16
F32 = jnp.float32
ANY = pl.BlockSpec(memory_space=pl.ANY)
SMEM = pl.BlockSpec(memory_space=pltpu.SMEM)
VM = pl.BlockSpec(memory_space=pltpu.VMEM)
LIMIT = 48 * 1024 * 1024


def pack(q, v, o, pieces):
    rq, cq = q.shape
    ro, co = o.shape
    a, b, r = rq // pieces, ro // pieces, co // cq

    def body(q_ref, v_ref, o_ref, *outs):
        for p in range(pieces):
            outs[p][0:a, :] = q_ref[p * a : (p + 1) * a, :].astype(BF)
            outs[p][a : 2 * a, :] = v_ref[p * a : (p + 1) * a, :].astype(BF)
            for c in range(r):
                outs[p][2 * a + c * b : 2 * a + (c + 1) * b, :] = o_ref[
                    p * b : (p + 1) * b, c * cq : (c + 1) * cq
                ].astype(BF)

    shape = jax.ShapeDtypeStruct((2 * a + r * b, cq), BF)
    return pl.pallas_call(
        body,
        out_shape=(shape,) * pieces,
        in_specs=[VM] * 3,
        out_specs=(VM,) * pieces,
        compiler_params=pltpu.CompilerParams(vmem_limit_bytes=LIMIT),
        name="pack",
    )(q, v, o)


def project(index, x, y, gq, gv, go, parts, n, m, rq, ro, rank):
    tokens = x.shape[0]
    steps = 4
    tt = tokens // steps
    cq, co = gq.shape[1], go.shape[1]
    cols = 2 * cq + co
    seg = rank // n
    aq, ao = rq // m, ro // m

    def body(index_ref, x_ref, y_ref, gq_ref, gv_ref, go_ref, *rest):
        part_refs = rest[:m]
        own_ref = rest[m]
        seg_refs = rest[m + 1 : m + n]
        bqv_ref, bo_ref, gram_ref = rest[m + n : m + n + 3]
        xs, ys, proj, sem_b, sem_o, sem_x, sem_y = rest[m + n + 3 :]
        for e in range(m):
            lane = index_ref[n + e]
            for d in range(n):
                row = index_ref[d]
                rows = pl.ds(pl.multiple_of(row * rq + lane * aq, aq), aq)
                pltpu.make_async_copy(
                    part_refs[e].at[d, pl.ds(0, aq), :], bqv_ref.at[rows, pl.ds(0, rank)], sem_b
                ).start()
                pltpu.make_async_copy(
                    part_refs[e].at[d, pl.ds(aq, aq), :], bqv_ref.at[rows, pl.ds(rank, rank)], sem_b
                ).start()
                rows = pl.ds(pl.multiple_of(row * ro + lane * ao, ao), ao)
                pltpu.make_async_copy(
                    part_refs[e].at[d, pl.ds(2 * aq, ao), :], bo_ref.at[rows, :], sem_o
                ).start()

        def copies(s):
            rows = pl.ds(s * tt, tt)
            return (
                pltpu.make_async_copy(x_ref.at[rows, :], xs.at[s], sem_x.at[s]),
                pltpu.make_async_copy(y_ref.at[rows, :], ys.at[s], sem_y.at[s]),
            )

        for s in range(steps):
            for copy in copies(s):
                copy.start()
        pltpu.make_async_copy(bqv_ref, bqv_ref, sem_b).wait()
        pltpu.make_async_copy(bo_ref, bo_ref, sem_o).wait()
        for s in range(steps):
            for copy in copies(s):
                copy.wait()
            rows = slice(s * tt, (s + 1) * tt)
            xb = jnp.dot(xs[s], bqv_ref[...], preferred_element_type=F32).T
            yb = jnp.dot(ys[s], bo_ref[...], preferred_element_type=F32).T
            for left, grad, lo, hi in (
                (xb[0:rank], gq_ref, 0, cq),
                (xb[rank : 2 * rank], gv_ref, cq, 2 * cq),
                (yb, go_ref, 2 * cq, cols),
            ):
                top = left.astype(BF)
                low = (left - top.astype(F32)).astype(BF)
                right = grad[rows, :]
                value = jnp.dot(top, right, preferred_element_type=F32) + jnp.dot(
                    low, right, preferred_element_type=F32
                )
                if s == 0:
                    proj[:, lo:hi] = value
                else:
                    proj[:, lo:hi] = proj[:, lo:hi] + value
        own_ref[...] = proj[pl.ds(pl.multiple_of(index_ref[0] * seg, seg), seg), :]
        for d in range(1, n):
            seg_refs[d - 1][...] = proj[
                pl.ds(pl.multiple_of(index_ref[d] * seg, seg), seg), :
            ].astype(BF)
        inner = (((0,), (0,)), ((), ()))
        both = lax.dot_general(bqv_ref[...], bqv_ref[...], inner, preferred_element_type=F32)
        gram_ref[0] = both[0:rank, 0:rank]
        gram_ref[1] = both[rank:, rank:]
        gram_ref[2] = lax.dot_general(bo_ref[...], bo_ref[...], inner, preferred_element_type=F32)

    outs = (
        [jax.ShapeDtypeStruct((seg, cols), F32)]
        + [jax.ShapeDtypeStruct((seg, cols), BF)] * (n - 1)
        + [
            jax.ShapeDtypeStruct((n * rq, 2 * rank), BF),
            jax.ShapeDtypeStruct((n * ro, rank), BF),
            jax.ShapeDtypeStruct((3, rank, rank), F32),
        ]
    )
    return pl.pallas_call(
        body,
        out_shape=tuple(outs),
        in_specs=[SMEM, ANY, ANY, VM, VM, VM] + [ANY] * m,
        out_specs=tuple([VM] * len(outs)),
        scratch_shapes=[
            pltpu.VMEM((steps, tt, x.shape[1]), BF),
            pltpu.VMEM((steps, tt, y.shape[1]), BF),
            pltpu.VMEM((rank, cols), F32),
            pltpu.SemaphoreType.DMA,
            pltpu.SemaphoreType.DMA,
            pltpu.SemaphoreType.DMA((steps,)),
            pltpu.SemaphoreType.DMA((steps,)),
        ],
        compiler_params=pltpu.CompilerParams(vmem_limit_bytes=LIMIT),
        name="project",
    )(index, x, y, gq, gv, go, *parts)


def halves(value):
    top = value.astype(BF)
    return top, (value - top.astype(F32)).astype(BF)


def moments(index, segs, means, squares, gram, n, rank):
    widths = [w.shape[1] for w in means]
    cols = sum(widths)
    seg = rank // n

    def body(index_ref, *rest):
        seg_refs = rest[:n]
        mean_refs = rest[n : n + 3]
        square_refs = rest[n + 3 : n + 6]
        gram_ref = rest[n + 6]
        first_refs = rest[n + 7 : n + 10]
        second_refs = rest[n + 10 : n + 13]
        top_ref, low_ref, sum_ref, proj = rest[n + 13 :]
        for d in range(n):
            proj[pl.ds(pl.multiple_of(index_ref[d] * seg, seg), seg), :] = seg_refs[d][...].astype(F32)
        at = 0
        total = jnp.zeros((1, 1), F32)
        for k in range(3):
            w = widths[k]
            value = proj[:, at : at + w]
            first = beta_first * mean_refs[k][...] + (1.0 - beta_first) * value
            second = beta_second * square_refs[k][...] + (1.0 - beta_second) * value * value
            first_refs[k][...] = first
            second_refs[k][...] = second
            direction = first / jnp.sqrt(second)
            top, low = halves(direction)
            top_ref[:, at : at + w] = top
            low_ref[:, at : at + w] = low
            g_top, g_low = halves(gram_ref[k])
            applied = (
                jnp.dot(g_top, top, preferred_element_type=F32)
                + jnp.dot(g_top, low, preferred_element_type=F32)
                + jnp.dot(g_low, top, preferred_element_type=F32)
            )
            total = total + jnp.sum(direction * applied, keepdims=True)
            at += w
        sum_ref[...] = jnp.broadcast_to(total, sum_ref.shape)

    outs = [jax.ShapeDtypeStruct((rank, w), F32) for w in widths] * 2 + [
        jax.ShapeDtypeStruct((rank, cols), BF),
        jax.ShapeDtypeStruct((rank, cols), BF),
        jax.ShapeDtypeStruct((8, 128), F32),
    ]
    return pl.pallas_call(
        body,
        out_shape=tuple(outs),
        in_specs=[SMEM] + [VM] * (n + 7),
        out_specs=tuple([VM] * len(outs)),
        scratch_shapes=[pltpu.VMEM((rank, cols), F32)],
        compiler_params=pltpu.CompilerParams(vmem_limit_bytes=LIMIT),
        name="moments",
    )(index, *segs, *means, *squares, gram)


def factor_of(sum_refs, count):
    values = [ref[0:1, 0:1] for ref in sum_refs]
    while len(values) > 1:
        values = [values[i] + values[i + 1] for i in range(0, len(values), 2)]
    return 1.0 / jnp.sqrt(values[0] / count + floor_mean)


def steps_of(rows, top, low, bqv, bo, sums, count, rq, ro, cq, co, rank):
    def body(index_ref, top_ref, low_ref, bqv_ref, bo_ref, *rest):
        sum_refs = rest[: len(sums)]
        q_ref, v_ref, o_ref = rest[len(sums) :]
        scale = -factor_of(sum_refs, count)

        def lowrank(basis, lo, hi):
            return jnp.dot(basis, top_ref[:, lo:hi], preferred_element_type=F32) + jnp.dot(
                basis, low_ref[:, lo:hi], preferred_element_type=F32
            )

        mine = pl.ds(pl.multiple_of(index_ref[0] * rq, rq), rq)
        q_ref[...] = scale * lowrank(bqv_ref[mine, 0:rank], 0, cq)
        v_ref[...] = scale * lowrank(bqv_ref[mine, rank : 2 * rank], cq, 2 * cq)
        mine = pl.ds(pl.multiple_of(index_ref[0] * ro, ro), ro)
        o_ref[...] = scale * lowrank(bo_ref[mine, :], 2 * cq, 2 * cq + co)

    outs = [jax.ShapeDtypeStruct((rq, cq), F32)] * 2 + [jax.ShapeDtypeStruct((ro, co), F32)]
    return pl.pallas_call(
        body,
        out_shape=tuple(outs),
        in_specs=[SMEM] + [VM] * (4 + len(sums)),
        out_specs=tuple([VM] * 3),
        compiler_params=pltpu.CompilerParams(vmem_limit_bytes=LIMIT),
        name="steps",
    )(rows, top, low, bqv, bo, *sums)


def write_copies(rows, labels, pieces, top, bqv, bo, sums, count, old, n, total, rq, ro, cq, co, rank):
    a, b, r = rq // total, ro // total, co // cq
    k = len(pieces)
    s = len(sums)

    def body(index_ref, top_ref, bqv_ref, bo_ref, *rest):
        sum_refs = rest[:s]
        piece_refs = rest[s : s + k]
        rest = rest[s + k + (3 if old else 0) :]
        q_out, v_out, o_out, q_buf, v_buf, o_buf, sem = rest
        scale = -learn_rate * factor_of(sum_refs, count)
        copies = []
        for i in range(k):
            piece = piece_refs[i]
            at = index_ref[i]
            here = pl.ds(pl.multiple_of(at * rq + labels[i] * a, a), a)
            there = pl.ds(pl.multiple_of(at * ro + labels[i] * b, b), b)
            low = jnp.dot(bqv_ref[here, 0:rank], top_ref[:, 0:cq], preferred_element_type=F32)
            q_buf[i] = (piece[0:a, :].astype(F32) + scale * low).astype(BF)
            copies.append(pltpu.make_async_copy(q_buf.at[i], q_out.at[here, :], sem.at[3 * i]))
            copies[-1].start()
            low = jnp.dot(
                bqv_ref[here, rank : 2 * rank], top_ref[:, cq : 2 * cq], preferred_element_type=F32
            )
            v_buf[i] = (piece[a : 2 * a, :].astype(F32) + scale * low).astype(BF)
            copies.append(pltpu.make_async_copy(v_buf.at[i], v_out.at[here, :], sem.at[3 * i + 1]))
            copies[-1].start()
            low = jnp.dot(bo_ref[there, :], top_ref[:, 2 * cq :], preferred_element_type=F32)
            for c in range(r):
                old_rows = piece[2 * a + c * b : 2 * a + (c + 1) * b, :].astype(F32)
                o_buf[i, :, c * cq : (c + 1) * cq] = (
                    old_rows + scale * low[:, c * cq : (c + 1) * cq]
                ).astype(BF)
            copies.append(pltpu.make_async_copy(o_buf.at[i], o_out.at[there, :], sem.at[3 * i + 2]))
            copies[-1].start()
        for copy in copies:
            copy.wait()

    outs = (
        jax.ShapeDtypeStruct((n * rq, cq), BF),
        jax.ShapeDtypeStruct((n * rq, cq), BF),
        jax.ShapeDtypeStruct((n * ro, co), BF),
    )
    before = 4 + s + k
    return pl.pallas_call(
        body,
        out_shape=outs,
        in_specs=[SMEM] + [VM] * (3 + s + k) + ([ANY] * 3 if old else []),
        out_specs=(ANY,) * 3,
        input_output_aliases={before + i: i for i in range(3)} if old else {},
        scratch_shapes=[
            pltpu.VMEM((k, a, cq), BF),
            pltpu.VMEM((k, a, cq), BF),
            pltpu.VMEM((k, b, co), BF),
            pltpu.SemaphoreType.DMA((3 * k,)),
        ],
        compiler_params=pltpu.CompilerParams(vmem_limit_bytes=LIMIT),
        name="copies",
    )(rows, top, bqv, bo, *sums, *pieces, *(old or ()))


def solution(mesh):
    n = mesh.shape["fs"]
    m = mesh.shape["tp"]
    order = list(range(0, n, 2)) + list(range(n - 1 - n % 2, 0, -2))
    place = [order.index(i) for i in range(n)]
    onward = [(order[i], order[(i + 1) % n]) for i in range(n)]
    back = [(d, s) for s, d in onward]

    def swap(x, axis, bits):
        size = mesh.shape[axis]
        return lax.ppermute(x, axis, [(i, i ^ bits) for i in range(size)])

    def local(x, y, gq, gv, go, wq, wv, wo, bq, bv, bo, mq, mv, mo, sq, sv, so):
        rq, cq = wq.shape
        ro, co = wo.shape
        rank = bq.shape[1]
        count = float(2 * n * rq * m * cq + n * ro * m * co)
        me = lax.axis_index("fs")
        lane = lax.axis_index("tp")
        pieces = 2 * STREAMS

        packed = pack(wq, wv, wo, pieces)

        aq, ao = rq // m, ro // m
        share = jnp.concatenate(
            [
                lax.dynamic_slice_in_dim(bq, lane * aq, aq, 0),
                lax.dynamic_slice_in_dim(bv, lane * aq, aq, 0),
                lax.dynamic_slice_in_dim(bo, lane * ao, ao, 0),
            ]
        )
        parts = [jnp.stack([share] + [swap(share, "fs", d) for d in range(1, n)])]
        offsets = [0]
        bit = m // 2
        while bit:
            parts = parts + [swap(part, "tp", bit) for part in parts]
            offsets = offsets + [e ^ bit for e in offsets]
            bit //= 2
        index = jnp.stack([me ^ d for d in range(n)] + [lane ^ e for e in offsets]).astype(jnp.int32)

        arrived = [[] for _ in range(n)]
        walk = jnp.asarray(order, jnp.int32)
        spot = jnp.asarray(place, jnp.int32)[me]
        arrived[0] = [(packed[p], p, me) for p in range(pieces)]
        for p in range(pieces):
            piece = packed[p]
            for k in range(1, n):
                piece = lax.ppermute(piece, "fs", back if p % 2 else onward)
                source = walk[(spot + k) % n] if p % 2 else walk[(spot - k) % n]
                arrived[k].append((piece, p, source))

        out = project(index, x, y, gq, gv, go, parts, n, m, rq, ro, rank)
        own, given, (bqv, bo_all, gram) = out[0], out[1:n], out[n:]
        total = own
        for d in range(1, n):
            total = total + swap(given[d - 1], "fs", d).astype(F32)
        total = total.astype(BF)
        segs = [total] + [swap(total, "fs", d) for d in range(1, n)]
        out = moments(index, segs, (mq, mv, mo), (sq, sv, so), gram, n, rank)
        firsts, seconds, (top, low, part_sum) = out[0:3], out[3:6], out[6:]
        sums = [part_sum] + [swap(part_sum, "tp", e) for e in range(1, m)]
        steps = steps_of(index, top, low, bqv, bo_all, sums, count, rq, ro, cq, co, rank)
        old = None
        cut = max(n - 3, 1)
        for group in [range(0, cut)] + [[k] for k in range(cut, n)]:
            some = [item for k in group for item in arrived[k]]
            rows = jnp.stack([item[2] for item in some]).astype(jnp.int32)
            old = write_copies(
                rows,
                [item[1] for item in some],
                [item[0] for item in some],
                top,
                bqv,
                bo_all,
                sums,
                count,
                old,
                n,
                pieces,
                rq,
                ro,
                cq,
                co,
                rank,
            )
        return (*steps, *old, *firsts, *seconds)

    rows = P("fs", None)
    both = P("fs", "tp")
    cols = P(None, "tp")
    return jax.shard_map(
        local,
        mesh=mesh,
        in_specs=(rows, rows) + (both,) * 6 + (rows,) * 3 + (cols,) * 6,
        out_specs=(both,) * 3 + (cols,) * 9,
        check_vma=False,
    )
```

```python
import jax
import jax.numpy as jnp
from jax import lax
from jax.experimental import pallas as pl
from jax.experimental.pallas import tpu as pltpu
from jax.sharding import PartitionSpec as P

beta_first = 0.8
beta_second = 0.9
floor_mean = 0.005
learn_rate = 0.05

STREAMS = 2
BF = jnp.bfloat16
F32 = jnp.float32
ANY = pl.BlockSpec(memory_space=pl.ANY)
SMEM = pl.BlockSpec(memory_space=pltpu.SMEM)
VM = pl.BlockSpec(memory_space=pltpu.VMEM)
MIB = 1024 * 1024


def params(mib):
    return pltpu.CompilerParams(vmem_limit_bytes=mib * MIB)


def cost(flops, moved):
    return pl.CostEstimate(flops=int(flops), bytes_accessed=int(moved), transcendentals=0)


def inner_size(n):
    size = 1
    while (2 * size) ** 2 <= n:
        size *= 2
    return size


def walk_at(i, n):
    return jnp.where(i < n // 2, 2 * i, 2 * (n - 1 - i) + 1)


def place_of(v, n):
    half = lax.shift_right_logical(v, 1)
    return jnp.where(lax.bitwise_and(v, 1) == 0, half, n - 1 - half)


def source_of(me, k, forward, n):
    place = place_of(me, n) + (n - k if forward else k)
    return walk_at(lax.rem(place, n), n)


def pack(q, v, o, pieces):
    rq, cq = q.shape
    ro, co = o.shape
    a, b, r = rq // pieces, ro // pieces, co // cq

    def body(q_hbm, v_hbm, o_hbm, *rest):
        outs, (q_ref, v_ref, o_ref, sem) = rest[:pieces], rest[pieces:]
        copies = []
        for p in range(pieces):
            some = []
            for i, (src, dst, h) in enumerate(((q_hbm, q_ref, a), (v_hbm, v_ref, a), (o_hbm, o_ref, b))):
                rows = pl.ds(p * h, h)
                some.append(pltpu.make_async_copy(src.at[rows, :], dst.at[rows, :], sem.at[p, i]))
                some[-1].start()
            copies.append(some)
        for p in range(pieces):
            for copy in copies[p]:
                copy.wait()
            outs[p][0:a, :] = q_ref[p * a : (p + 1) * a, :].astype(BF)
            outs[p][a : 2 * a, :] = v_ref[p * a : (p + 1) * a, :].astype(BF)
            for c in range(r):
                outs[p][2 * a + c * b : 2 * a + (c + 1) * b, :] = o_ref[
                    p * b : (p + 1) * b, c * cq : (c + 1) * cq
                ].astype(BF)

    shape = jax.ShapeDtypeStruct((2 * a + r * b, cq), BF)
    return pl.pallas_call(
        body,
        out_shape=(shape,) * pieces,
        in_specs=[ANY] * 3,
        out_specs=(VM,) * pieces,
        scratch_shapes=[
            pltpu.VMEM((rq, cq), F32),
            pltpu.VMEM((rq, cq), F32),
            pltpu.VMEM((ro, co), F32),
            pltpu.SemaphoreType.DMA((pieces, 3)),
        ],
        compiler_params=params(8),
        name="pack",
    )(q, v, o)


def project(index, x, y, gq, gv, go, parts, offsets, n, m, rq, ro, rank):
    tokens = x.shape[0]
    steps = 2
    tt = tokens // steps
    cq, co = gq.shape[1], go.shape[1]
    cols = 2 * cq + co
    seg = rank // n
    aq, ao = rq // m, ro // m
    near = inner_size(n)
    far = n // near

    def body(index_ref, x_ref, y_ref, gq_ref, gv_ref, go_ref, *rest):
        part_refs = rest[:m]
        keep_ref = rest[m]
        send_refs = rest[m + 1 : m + near]
        bqv_ref, bo_ref, gram_ref = rest[m + near : m + near + 3]
        xs, ys, gqs, gvs, gos, proj, sem_b, sem_o, sem_x = rest[m + near + 3 :]
        me, lane = index_ref[0], index_ref[1]
        for e in range(m):
            share = lax.bitwise_xor(lane, offsets[e])
            for d in range(n):
                row = lax.bitwise_xor(me, d)
                rows = pl.ds(pl.multiple_of(row * rq + share * aq, aq), aq)
                pltpu.make_async_copy(
                    part_refs[e].at[d, pl.ds(0, aq), :], bqv_ref.at[rows, pl.ds(0, rank)], sem_b
                ).start()
                pltpu.make_async_copy(
                    part_refs[e].at[d, pl.ds(aq, aq), :], bqv_ref.at[rows, pl.ds(rank, rank)], sem_b
                ).start()
                rows = pl.ds(pl.multiple_of(row * ro + share * ao, ao), ao)
                pltpu.make_async_copy(
                    part_refs[e].at[d, pl.ds(2 * aq, ao), :], bo_ref.at[rows, :], sem_o
                ).start()

        copies = []
        for s in range(steps):
            some = []
            for i, (src, dst) in enumerate(
                ((x_ref, xs), (y_ref, ys), (gq_ref, gqs), (gv_ref, gvs), (go_ref, gos))
            ):
                rows = pl.ds(s * tt, tt)
                some.append(pltpu.make_async_copy(src.at[rows, :], dst.at[rows, :], sem_x.at[s, i]))
                some[-1].start()
            copies.append(some)
        pltpu.make_async_copy(bqv_ref, bqv_ref, sem_b).wait()
        pltpu.make_async_copy(bo_ref, bo_ref, sem_o).wait()
        for s in range(steps):
            rows = slice(s * tt, (s + 1) * tt)
            copies[s][0].wait()
            xb = jnp.dot(xs[rows, :], bqv_ref[...], preferred_element_type=F32).T
            copies[s][1].wait()
            yb = jnp.dot(ys[rows, :], bo_ref[...], preferred_element_type=F32).T
            for copy in copies[s][2:]:
                copy.wait()
            for left, grad, lo, hi in (
                (xb[0:rank], gqs, 0, cq),
                (xb[rank : 2 * rank], gvs, cq, 2 * cq),
                (yb, gos, 2 * cq, cols),
            ):
                top, low = halves(left)
                right = grad[rows, :]
                value = jnp.dot(top, right, preferred_element_type=F32) + jnp.dot(
                    low, right, preferred_element_type=F32
                )
                if s == 0:
                    proj[:, lo:hi] = value
                else:
                    proj[:, lo:hi] = proj[:, lo:hi] + value
        for e in range(near):
            for k in range(far):
                row = lax.bitwise_xor(me, e + near * k)
                block = proj[pl.ds(pl.multiple_of(row * seg, seg), seg), :]
                if e == 0:
                    keep_ref[k * seg : (k + 1) * seg, :] = block
                else:
                    send_refs[e - 1][k * seg : (k + 1) * seg, :] = block.astype(BF)
        inner = (((0,), (0,)), ((), ()))
        both = lax.dot_general(bqv_ref[...], bqv_ref[...], inner, preferred_element_type=F32)
        gram_ref[0] = both[0:rank, 0:rank]
        gram_ref[1] = both[rank:, rank:]
        gram_ref[2] = lax.dot_general(bo_ref[...], bo_ref[...], inner, preferred_element_type=F32)

    outs = (
        [jax.ShapeDtypeStruct((far * seg, cols), F32)]
        + [jax.ShapeDtypeStruct((far * seg, cols), BF)] * (near - 1)
        + [
            jax.ShapeDtypeStruct((n * rq, 2 * rank), BF),
            jax.ShapeDtypeStruct((n * ro, rank), BF),
            jax.ShapeDtypeStruct((3, rank, rank), F32),
        ]
    )
    return pl.pallas_call(
        body,
        out_shape=tuple(outs),
        in_specs=[SMEM] + [ANY] * (5 + m),
        out_specs=tuple([VM] * len(outs)),
        scratch_shapes=[
            pltpu.VMEM(x.shape, BF),
            pltpu.VMEM(y.shape, BF),
            pltpu.VMEM(gq.shape, BF),
            pltpu.VMEM(gv.shape, BF),
            pltpu.VMEM(go.shape, BF),
            pltpu.VMEM((rank, cols), F32),
            pltpu.SemaphoreType.DMA,
            pltpu.SemaphoreType.DMA,
            pltpu.SemaphoreType.DMA((steps, 5)),
        ],
        compiler_params=params(28),
        cost_estimate=cost(2 * tokens * (n * rq * 2 * rank + n * ro * rank + 2 * rank * cols), 16 * MIB),
        name="project",
    )(index, x, y, gq, gv, go, *parts)


def halves(value):
    top = value.astype(BF)
    return top, (value - top.astype(F32)).astype(BF)


def moments(index, segs, means, squares, gram, n, rank):
    widths = [w.shape[1] for w in means]
    cols = sum(widths)
    seg = rank // n
    near = inner_size(n)
    far = n // near

    def body(index_ref, *rest):
        seg_refs = rest[:near]
        sources = rest[near : near + 6]
        gram_ref = rest[near + 6]
        outs = rest[near + 7 : near + 16]
        firsts, seconds, (top_ref, low_ref, sum_ref) = outs[0:3], outs[3:6], outs[6:9]
        proj = rest[near + 16]
        held = rest[near + 17 : near + 23]
        sem_in, = rest[near + 23 :]
        loads = [pltpu.make_async_copy(sources[i], held[i], sem_in.at[i]) for i in range(6)]
        for copy in loads:
            copy.start()
        me = index_ref[0]
        for e in range(near):
            for k in range(far):
                row = lax.bitwise_xor(me, e + near * k)
                proj[pl.ds(pl.multiple_of(row * seg, seg), seg), :] = seg_refs[e][
                    k * seg : (k + 1) * seg, :
                ].astype(F32)
        at = 0
        total = jnp.zeros((1, 1), F32)
        for k in range(3):
            w = widths[k]
            loads[k].wait()
            loads[k + 3].wait()
            value = proj[:, at : at + w]
            first = beta_first * held[k][...] + (1.0 - beta_first) * value
            second = beta_second * held[k + 3][...] + (1.0 - beta_second) * value * value
            firsts[k][...] = first
            seconds[k][...] = second
            direction = first / jnp.sqrt(second)
            top, low = halves(direction)
            top_ref[:, at : at + w] = top
            low_ref[:, at : at + w] = low
            g_top, g_low = halves(gram_ref[k])
            applied = (
                jnp.dot(g_top, top, preferred_element_type=F32)
                + jnp.dot(g_top, low, preferred_element_type=F32)
                + jnp.dot(g_low, top, preferred_element_type=F32)
            )
            total = total + jnp.sum(direction * applied, keepdims=True)
            at += w
        sum_ref[...] = jnp.broadcast_to(total, sum_ref.shape)

    outs = [jax.ShapeDtypeStruct((rank, w), F32) for w in widths] * 2 + [
        jax.ShapeDtypeStruct((rank, cols), BF),
        jax.ShapeDtypeStruct((rank, cols), BF),
        jax.ShapeDtypeStruct((8, 128), F32),
    ]
    return pl.pallas_call(
        body,
        out_shape=tuple(outs),
        in_specs=[SMEM] + [VM] * near + [ANY] * 6 + [VM],
        out_specs=tuple([VM] * len(outs)),
        scratch_shapes=[pltpu.VMEM((rank, cols), F32)]
        + [pltpu.VMEM((rank, w), F32) for w in widths] * 2
        + [pltpu.SemaphoreType.DMA((6,))],
        compiler_params=params(12),
        cost_estimate=cost(10**9, 4 * MIB),
        name="moments",
    )(index, *segs, *means, *squares, gram)


def factor_of(sum_refs, count):
    values = [ref[0:1, 0:1] for ref in sum_refs]
    while len(values) > 1:
        values = [values[i] + values[i + 1] for i in range(0, len(values), 2)]
    return 1.0 / jnp.sqrt(values[0] / count + floor_mean)


def steps_of(index, top, low, bqv, bo, sums, count, rq, ro, cq, co, rank):
    def body(index_ref, top_ref, low_ref, bqv_hbm, bo_hbm, *rest):
        sum_refs = rest[: len(sums)]
        q_ref, v_ref, o_ref, bqv_ref, bo_ref, sem = rest[len(sums) :]
        mine = pl.ds(pl.multiple_of(index_ref[0] * rq, rq), rq)
        load_qv = pltpu.make_async_copy(bqv_hbm.at[mine, :], bqv_ref, sem.at[0])
        load_qv.start()
        mine = pl.ds(pl.multiple_of(index_ref[0] * ro, ro), ro)
        load_o = pltpu.make_async_copy(bo_hbm.at[mine, :], bo_ref, sem.at[1])
        load_o.start()
        scale = -factor_of(sum_refs, count)

        def lowrank(basis, lo, hi):
            return jnp.dot(basis, top_ref[:, lo:hi], preferred_element_type=F32) + jnp.dot(
                basis, low_ref[:, lo:hi], preferred_element_type=F32
            )

        load_qv.wait()
        q_ref[...] = scale * lowrank(bqv_ref[:, 0:rank], 0, cq)
        v_ref[...] = scale * lowrank(bqv_ref[:, rank : 2 * rank], cq, 2 * cq)
        load_o.wait()
        o_ref[...] = scale * lowrank(bo_ref[...], 2 * cq, 2 * cq + co)

    outs = [jax.ShapeDtypeStruct((rq, cq), F32)] * 2 + [jax.ShapeDtypeStruct((ro, co), F32)]
    return pl.pallas_call(
        body,
        out_shape=tuple(outs),
        in_specs=[SMEM, VM, VM, ANY, ANY] + [VM] * len(sums),
        out_specs=tuple([VM] * 3),
        scratch_shapes=[
            pltpu.VMEM((rq, 2 * rank), BF),
            pltpu.VMEM((ro, rank), BF),
            pltpu.SemaphoreType.DMA((2,)),
        ],
        compiler_params=params(8),
        cost_estimate=cost(10**9, 4 * MIB),
        name="steps",
    )(index, top, low, bqv, bo, *sums)


def write_copies(index, labels, pieces, top, bqv, bo, sums, count, old, n, total, rq, ro, cq, co, rank):
    a, b, r = rq // total, ro // total, co // cq
    k = len(pieces)
    s = len(sums)

    def body(index_ref, top_ref, bqv_hbm, bo_hbm, *rest):
        sum_refs = rest[:s]
        piece_refs = rest[s : s + k]
        rest = rest[s + k + (3 if old else 0) :]
        q_out, v_out, o_out, buf, bqv_ref, bo_ref, sem_b, sem_in, sem_out = rest
        me = index_ref[0]
        heres, theres, basis, loads = [], [], [], []
        for i, (p, step) in enumerate(labels):
            at = source_of(me, step, p % 2 == 0, n)
            heres.append(pl.ds(pl.multiple_of(at * rq + p * a, a), a))
            theres.append(pl.ds(pl.multiple_of(at * ro + p * b, b), b))
            basis.append(
                (
                    pltpu.make_async_copy(bqv_hbm.at[heres[i], :], bqv_ref.at[i], sem_b.at[i, 0]),
                    pltpu.make_async_copy(bo_hbm.at[theres[i], :], bo_ref.at[i], sem_b.at[i, 1]),
                )
            )
            loads.append(pltpu.make_async_copy(piece_refs[i], buf.at[i], sem_in.at[i]))
            for copy in basis[i]:
                copy.start()
            loads[i].start()
        scale = -learn_rate * factor_of(sum_refs, count)
        copies = []

        def update(i, rows, value, target):
            buf[i, rows, :] = (buf[i, rows, :].astype(F32) + scale * value).astype(BF)
            copies.append(pltpu.make_async_copy(buf.at[i, rows, :], target, sem_out.at[i, len(copies) % (2 + r)]))
            copies[-1].start()

        for i in range(k):
            for copy in basis[i]:
                copy.wait()
            loads[i].wait()
            value = jnp.dot(bqv_ref[i, :, 0:rank], top_ref[:, 0:cq], preferred_element_type=F32)
            update(i, pl.ds(0, a), value, q_out.at[heres[i], :])
            value = jnp.dot(
                bqv_ref[i, :, rank : 2 * rank], top_ref[:, cq : 2 * cq], preferred_element_type=F32
            )
            update(i, pl.ds(a, a), value, v_out.at[heres[i], :])
            for c in range(r):
                value = jnp.dot(
                    bo_ref[i], top_ref[:, (2 + c) * cq : (3 + c) * cq], preferred_element_type=F32
                )
                update(i, pl.ds(2 * a + c * b, b), value, o_out.at[theres[i], pl.ds(c * cq, cq)])
        for copy in copies:
            copy.wait()

    outs = (
        jax.ShapeDtypeStruct((n * rq, cq), BF),
        jax.ShapeDtypeStruct((n * rq, cq), BF),
        jax.ShapeDtypeStruct((n * ro, co), BF),
    )
    before = 4 + s + k
    return pl.pallas_call(
        body,
        out_shape=outs,
        in_specs=[SMEM, VM, ANY, ANY] + [VM] * s + [ANY] * k + ([ANY] * 3 if old else []),
        out_specs=(ANY,) * 3,
        input_output_aliases={before + i: i for i in range(3)} if old else {},
        scratch_shapes=[
            pltpu.VMEM((k,) + pieces[0].shape, BF),
            pltpu.VMEM((k, a, 2 * rank), BF),
            pltpu.VMEM((k, b, rank), BF),
            pltpu.SemaphoreType.DMA((k, 2)),
            pltpu.SemaphoreType.DMA((k,)),
            pltpu.SemaphoreType.DMA((k, 2 + r)),
        ],
        compiler_params=params(20),
        cost_estimate=cost(k * 10**8, k * MIB),
        name="copies",
    )(index, top, bqv, bo, *sums, *pieces, *(old or ()))


def solution(mesh):
    n = mesh.shape["fs"]
    m = mesh.shape["tp"]
    near = inner_size(n)
    far = n // near
    order = [2 * i if i < n // 2 else 2 * (n - 1 - i) + 1 for i in range(n)]
    onward = [(order[i], order[(i + 1) % n]) for i in range(n)]
    back = [(d, s) for s, d in onward]

    def swap(x, axis, bits):
        size = mesh.shape[axis]
        return lax.ppermute(x, axis, [(i, i ^ bits) for i in range(size)])

    def local(x, y, gq, gv, go, wq, wv, wo, bq, bv, bo, mq, mv, mo, sq, sv, so):
        rq, cq = wq.shape
        ro, co = wo.shape
        rank = bq.shape[1]
        seg = rank // n
        count = float(2 * n * rq * m * cq + n * ro * m * co)
        me = lax.axis_index("fs")
        lane = lax.axis_index("tp")
        index = jnp.stack([me, lane]).astype(jnp.int32)
        pieces = 2 * STREAMS

        packed = pack(wq, wv, wo, pieces)
        arrived = [[(packed[p], (p, 0)) for p in range(pieces)]] + [[] for _ in range(n - 1)]
        for p in range(pieces):
            piece = packed[p]
            for k in range(1, n):
                piece = lax.ppermute(piece, "fs", back if p % 2 else onward)
                arrived[k].append((piece, (p, k)))

        aq, ao = rq // m, ro // m
        share = jnp.concatenate(
            [
                lax.dynamic_slice_in_dim(bq, lane * aq, aq, 0),
                lax.dynamic_slice_in_dim(bv, lane * aq, aq, 0),
                lax.dynamic_slice_in_dim(bo, lane * ao, ao, 0),
            ]
        )
        some = jnp.stack([share] + [swap(share, "fs", d) for d in range(1, near)])
        parts = [jnp.concatenate([some] + [swap(some, "fs", near * k) for k in range(1, far)])]
        offsets = [0]
        bit = m // 2
        while bit:
            parts = parts + [swap(part, "tp", bit) for part in parts]
            offsets = offsets + [e ^ bit for e in offsets]
            bit //= 2

        out = project(index, x, y, gq, gv, go, parts, offsets, n, m, rq, ro, rank)
        total, given, (bqv, bo_all, gram) = out[0], out[1:near], out[near:]
        for e in range(1, near):
            total = total + swap(given[e - 1], "fs", e).astype(F32)
        block = total[0:seg]
        for k in range(1, far):
            other = swap(total[k * seg : (k + 1) * seg].astype(BF), "fs", near * k)
            block = block + other.astype(F32)
        block = block.astype(BF)
        blocks = jnp.concatenate([block] + [swap(block, "fs", near * k) for k in range(1, far)])
        segs = [blocks] + [swap(blocks, "fs", e) for e in range(1, near)]

        out = moments(index, segs, (mq, mv, mo), (sq, sv, so), gram, n, rank)
        firsts, seconds, (top, low, part_sum) = out[0:3], out[3:6], out[6:]
        sums = [part_sum] + [swap(part_sum, "tp", e) for e in range(1, m)]
        steps = steps_of(index, top, low, bqv, bo_all, sums, count, rq, ro, cq, co, rank)

        groups = [sum(arrived[: n - 2], []), arrived[n - 2]]
        groups += [arrived[n - 1][2 * i : 2 * i + 2] for i in range(STREAMS)]
        old = None
        for group in groups:
            old = write_copies(
                index,
                [label for _, label in group],
                [piece for piece, _ in group],
                top,
                bqv,
                bo_all,
                sums,
                count,
                old,
                n,
                pieces,
                rq,
                ro,
                cq,
                co,
                rank,
            )
        return (*steps, *old, *firsts, *seconds)

    rows = P("fs", None)
    both = P("fs", "tp")
    cols = P(None, "tp")
    return jax.shard_map(
        local,
        mesh=mesh,
        in_specs=(rows, rows) + (both,) * 6 + (rows,) * 3 + (cols,) * 6,
        out_specs=(both,) * 3 + (cols,) * 9,
        check_vma=False,
    )
```
